32 devices in a mesh: rep: 2 (over y), fs: 4 (over z), tp: 4 (over x, core).
Axes of the slice: x: 2, y: 2, z: 4, core: 2. Of those that a mesh axis runs over, the one named last changes fastest.
Arguments:
- tokens: bfloat16 [4096, 2048], P(('rep', 'fs')), may hold values from -6 to 6
- norm_gain: float32 [2048], replicated, may hold values from 0.1 to 1.9
- up_weight: bfloat16 [2048, 4096], P('fs', 'tp'), may hold values from -0.125 to 0.125
- down_weight: bfloat16 [4096, 2048], P('tp', 'fs'), may hold values from -0.09375 to 0.09375
Outputs:
- result: bfloat16 [4096, 2048], P(('rep', 'fs', 'tp'))
The draws below stay inside these ranges and needn't reach their ends.
All inputs are finite; a program needn't handle non-finite values.
Results may differ from the reference program's by a relative error of at most 0.012.
Values may be sent and summed in bfloat16 or wider, within the bound.
A program may use at most 64 MiB of HBM per device.

```python
import jax
import jax.numpy as jnp
from jax import lax

D = 2048
FF = 4096
TOKENS = 4096
N_TP = 4


def block_scale(own_key, dims, split, smallest, largest):
    loudness = 1.0
    for axis_at, parts in split:
        draws = jax.random.uniform(jax.random.fold_in(jax.random.fold_in(own_key, 6), axis_at), (parts,), jnp.float32, smallest / len(split), largest / len(split))
        loudness = loudness * jnp.repeat(jnp.exp(draws), dims[axis_at] // parts).reshape((-1,) + (1,) * (len(dims) - 1 - axis_at))
    return loudness


def normal_values(key, shape, spread, most, pieces=(), held_as=jnp.bfloat16):
    level = block_scale(key, shape, pieces, -0.22, 0.18) if pieces else 1.0
    drawn = jax.random.normal(key, shape, jnp.float32) * spread * level
    return jnp.minimum(jnp.maximum(drawn, -most), most).astype(held_as)


def setup_inputs(seed: int = 0) -> dict:
    key_list = jax.random.split(jax.random.key(seed), 5)
    return {
        "tokens": normal_values(key_list[0], (TOKENS, D), 1.0, 6.0, ((0, 8),)),
        "norm_gain": jnp.clip(1.0 + 0.18 * jax.random.normal(key_list[1], (D,), jnp.float32), 0.1, 1.9),
        "up_weight": normal_values(key_list[2], (D, FF), D ** -0.5, 0.125, ((0, 4), (1, 4))),
        "down_weight": normal_values(key_list[3], (FF, D), FF ** -0.5, 0.09375, ((0, 4), (1, 4))),
    }


EPS = 1e-06

def reference(tokens, norm_gain, up_weight, down_weight):
    xf = tokens.astype(jnp.float32)
    scale = lax.rsqrt(lax.optimization_barrier(jnp.mean(xf * xf, axis=-1, keepdims=True)) + EPS)
    normed = (xf * scale * norm_gain.astype(jnp.float32)).astype(jnp.bfloat16)
    lifted = jnp.dot(normed, up_weight, preferred_element_type=jnp.float32)
    hidden = jnp.square(jnp.maximum(lifted, 0.0)).astype(jnp.bfloat16)
    block = FF // N_TP
    total = xf
    for index in range(N_TP):
        part = jnp.dot(hidden[:, index * block:(index + 1) * block], down_weight[index * block:(index + 1) * block, :], preferred_element_type=jnp.float32)
        rounded = lax.optimization_barrier(part.astype(jnp.bfloat16))
        total = total + rounded.astype(jnp.float32)
    return total.astype(jnp.bfloat16)
```

```python
import functools

import jax
import jax.numpy as jnp
from jax import lax
from jax.experimental import pallas as pl
from jax.experimental.pallas import tpu as pltpu
from jax.sharding import PartitionSpec as P

EPS = 1e-06
UP_CHUNKS = 2
CHUNK_COLS = 256


def shards(tokens, norm_gain, up_weight, down_weight):
    xf = tokens.astype(jnp.float32)
    scale = lax.rsqrt(jnp.mean(xf * xf, axis=-1, keepdims=True) + EPS)
    normed = (xf * scale * norm_gain).astype(jnp.bfloat16)
    rows = tokens.shape[0]
    halves = lax.axis_size("rep")
    share = up_weight.shape[0] // halves
    mine = lax.dynamic_slice_in_dim(up_weight, lax.axis_index("rep") * share, share, 0)
    arranged = normed.reshape(rows, -1, halves, share).transpose(0, 2, 1, 3).reshape(rows, -1)
    lifted = jnp.dot(
        arranged,
        lax.all_gather(mine, ("rep", "fs"), axis=0, tiled=True),
        preferred_element_type=jnp.float32,
    )
    width = down_weight.shape[1] // halves
    down_mine = lax.dynamic_slice_in_dim(down_weight, lax.axis_index("rep") * width, width, 1)
    collected = lax.all_gather(down_mine, ("rep", "fs"), axis=1, tiled=True)
    hidden_rows = collected.shape[0]
    down_block = (
        collected.reshape(hidden_rows, halves, -1, width)
        .transpose(0, 2, 1, 3)
        .reshape(hidden_rows, -1)
    )
    hidden = jnp.square(jnp.maximum(lifted, 0.0)).astype(jnp.bfloat16)
    own_rows = rows // lax.axis_size("tp")
    summed = lax.psum_scatter(
        jnp.dot(hidden, down_block, preferred_element_type=jnp.float32).astype(jnp.bfloat16),
        "tp",
        scatter_dimension=0,
        tiled=True,
    ).astype(jnp.float32)
    residual = lax.dynamic_slice_in_dim(xf, lax.axis_index("tp") * own_rows, own_rows, 0)
    return (residual + summed).astype(jnp.bfloat16)


def kernel(
    n, tok_hbm, gain_ref, up_hbm, dn_hbm, out_hbm,
    tok, nrm, upw, dnw, hid, acc, keep, asend, arecv, bsend, brecv, outv,
    up_send, up_recv, dn_send, dn_recv, tok_send, tok_recv,
    a_send, a_recv, b_send, b_recv, local, out_sem,
):
    y, z, t = lax.axis_index("rep"), lax.axis_index("fs"), lax.axis_index("tp")
    x, core = t // 2, t % 2
    partner = x * 2 + (1 - core)
    rows = tok_hbm.shape[0]
    own_rows = rows // 4
    up_rows = up_hbm.shape[0]
    H = upw.shape[1]
    CW = dnw.shape[2]
    DC = dn_hbm.shape[1] // CW
    UC = UP_CHUNKS
    piece = up_rows // UC
    half = rows // 2
    total = n * DC

    def at(yy, zz, tt):
        return {"rep": yy, "fs": zz, "tp": tt}

    def remote(src, dst, send, recv, where):
        return pltpu.make_async_remote_copy(
            src_ref=src, dst_ref=dst, send_sem=send, recv_sem=recv,
            device_id=where, device_id_type=pl.DeviceIdType.MESH,
        )

    def beside(side):
        return at(y, z - 1 if side == 0 else z + 1, t)

    def up_slot(s, c):
        return upw.at[pl.ds(pl.multiple_of(s * up_rows + c * piece, piece), piece), :]

    def up_own(c):
        return up_hbm.at[pl.ds(c * piece, piece), pl.ds(pl.multiple_of(y * H, H), H)]

    def dn_own(c):
        return dn_hbm.at[pl.ds(pl.multiple_of(y * H, H), H), pl.ds(c * CW, CW)]

    def up_copy(side, s, c, src):
        return remote(src, up_slot(s, c), up_send.at[side, s * UC + c],
                      up_recv.at[s * UC + c], beside(side))

    def dn_copy(side, s, c, src):
        return remote(src, dnw.at[s * DC + c], dn_send.at[side, s * DC + c],
                      dn_recv.at[s * DC + c], beside(side))

    def send_own_dn(side):
        for c in range(DC):
            dn_copy(side, z, c, dn_own(c)).start()

    def source(p):
        m = jnp.minimum(z, n - 1 - z)
        k = jnp.where(p <= 2 * m, (p + 1) // 2, p - m)
        sign = jnp.where(
            p <= 2 * m, jnp.where(p % 2 == 1, 1, -1), jnp.where(z < n - 1 - z, 1, -1)
        )
        return z + sign * k

    loads = [pltpu.make_async_copy(tok_hbm, tok.at[y], local.at[0])]
    for c in range(UC):
        loads.append(pltpu.make_async_copy(up_own(c), up_slot(z, c), local.at[1 + c]))
    for c in range(DC):
        loads.append(pltpu.make_async_copy(dn_own(c), dnw.at[z * DC + c], local.at[1 + UC + c]))
    for load in loads:
        load.start()

    peers = [at(y, z, partner)]
    for j in (1, 2, 3):
        peers.append(at((y + j // 2) % 2, z, ((x + j % 2) % 2) * 2 + core))
    barrier = pltpu.get_barrier_semaphore()
    for peer in peers:
        pl.semaphore_signal(barrier, inc=1, device_id=peer, device_id_type=pl.DeviceIdType.MESH)
    has = (z > 0, z < n - 1)
    for side in (0, 1):
        @pl.when(has[side])
        def _():
            pl.semaphore_signal(
                barrier, inc=1, device_id=beside(side), device_id_type=pl.DeviceIdType.MESH
            )
    greeted = 4 + jnp.where(has[0], 1, 0) + jnp.where(has[1], 1, 0)
    pl.semaphore_wait(barrier, greeted)

    for side in (0, 1):
        @pl.when(has[side])
        def _():
            for c in range(UC):
                up_copy(side, z, c, up_own(c)).start()

    part = pl.ds(pl.multiple_of(core * half, half), half)
    across = remote(tok_hbm.at[part, :], tok.at[y, part, :], tok_send.at[0], tok_recv.at[0],
                    at(1 - y, z, t))
    across.start()

    @pl.when(z == 0)
    def _():
        send_own_dn(1)

    @pl.when(z == n - 1)
    def _():
        send_own_dn(0)

    gain = gain_ref[...]

    def normalise(yy):
        def tile(i, carry):
            xf = tok[yy, pl.ds(pl.multiple_of(i * own_rows, own_rows), own_rows), :].astype(jnp.float32)
            scale = lax.rsqrt(jnp.mean(xf * xf, axis=-1, keepdims=True) + EPS)
            to = (i % 2) * rows + (yy * 2 + i // 2) * own_rows
            nrm[pl.ds(pl.multiple_of(to, own_rows), own_rows), :] = (xf * scale * gain).astype(jnp.bfloat16)
            return carry
        lax.fori_loop(0, 4, tile, 0)

    loads[0].wait()
    normalise(y)

    for p in range(1, n):
        s = source(p)
        for c in range(UC):
            up_copy(0, s, c, up_slot(s, c)).wait_recv()
            for side in (0, 1):
                @pl.when(((s > z) if side == 0 else (s < z)) & has[side])
                def _():
                    up_copy(side, s, c, up_slot(s, c)).start()
        for side in (0, 1):
            @pl.when((s == (n - 1 if side == 0 else 0)) & has[side])
            def _():
                send_own_dn(side)

    theirs = pl.ds(pl.multiple_of((1 - core) * half, half), half)
    across.wait_recv()
    over = remote(tok.at[1 - y, part, :], tok.at[1 - y, part, :], tok_send.at[1], tok_recv.at[1],
                  at(y, z, partner))
    over.start()
    remote(tok.at[1 - y, theirs, :], tok.at[1 - y, theirs, :], tok_send.at[1], tok_recv.at[1],
           at(y, z, partner)).wait_recv()
    normalise(1 - y)
    for load in loads[1:]:
        load.wait()

    def lift(i, carry):
        r = pl.ds(pl.multiple_of(i * half, half), half)
        lifted = jnp.dot(nrm[r, :], upw[...], preferred_element_type=jnp.float32)
        hid[r, :] = jnp.square(jnp.maximum(lifted, 0.0)).astype(jnp.bfloat16)
        return carry

    lax.fori_loop(0, 2 * rows // half, lift, 0)

    own_q = y * 2 + x

    def a_copy(i):
        return remote(asend.at[i], arecv.at[i], a_send.at[i], a_recv.at[i], at(y, z, partner))

    def b_copy(i, j):
        yy, xx = (y + j // 2) % 2, (x + j % 2) % 2
        return remote(bsend.at[i, yy * 2 + xx], brecv.at[i, j - 1], b_send.at[i, j - 1],
                      b_recv.at[i, j - 1], at(yy, z, xx * 2 + core))

    def out_copy(i):
        column = (source(i // DC) * DC + i % DC) * CW
        return pltpu.make_async_copy(
            outv.at[i], out_hbm.at[:, pl.ds(pl.multiple_of(column, CW), CW)], out_sem.at[i]
        )

    def finish(i):
        for j in (1, 2, 3):
            b_copy(i, j).wait_recv()
        column = (source(i // DC) * DC + i % DC) * CW
        res = tok[y, pl.ds(pl.multiple_of(t * own_rows, own_rows), own_rows),
                  pl.ds(pl.multiple_of(column, CW), CW)].astype(jnp.float32)
        res = res + keep[i]
        for j in range(3):
            res = res + brecv[i, j].astype(jnp.float32)
        outv[i] = res.astype(jnp.bfloat16)
        out_copy(i).start()

    def step(i, carry):
        p, c = i // DC, i % DC
        s = source(p)

        @pl.when(p > 0)
        def _():
            dn_copy(0, s, c, dnw.at[s * DC + c]).wait_recv()
            for side in (0, 1):
                @pl.when(((s > z) if side == 0 else (s < z)) & has[side])
                def _():
                    dn_copy(side, s, c, dnw.at[s * DC + c]).start()

        block = dnw[s * DC + c]
        first = hid[pl.ds(pl.multiple_of((1 - core) * rows, rows), rows), :]
        asend[i] = jnp.dot(first, block, preferred_element_type=jnp.float32).astype(jnp.bfloat16)
        a_copy(i).start()
        second = hid[pl.ds(pl.multiple_of(core * rows, rows), rows), :]
        acc[...] = jnp.dot(second, block, preferred_element_type=jnp.float32)
        a_copy(i).wait_recv()
        for q in range(4):
            r = pl.ds(q * own_rows, own_rows)
            bsend[i, q] = (acc[r, :] + arecv[i, r, :].astype(jnp.float32)).astype(jnp.bfloat16)
        for j in (3, 2, 1):
            b_copy(i, j).start()
        r = pl.ds(pl.multiple_of(own_q * own_rows, own_rows), own_rows)
        keep[i] = acc[r, :] + arecv[i, r, :].astype(jnp.float32)

        @pl.when(i > 0)
        def _():
            finish(i - 1)
        return carry

    lax.fori_loop(0, total, step, 0)
    finish(total - 1)

    across.wait_send()
    over.wait_send()

    def drain(i, carry):
        a_copy(i).wait_send()
        for j in (1, 2, 3):
            b_copy(i, j).wait_send()
        out_copy(i).wait()
        return carry

    lax.fori_loop(0, total, drain, 0)
    for side in (0, 1):
        for s in range(n):
            @pl.when(((z <= s) if side == 0 else (z >= s)) & has[side])
            def _():
                for c in range(UC):
                    up_copy(side, s, c, up_slot(s, c)).wait_send()
                for c in range(DC):
                    dn_copy(side, s, c, dnw.at[s * DC + c]).wait_send()


def fused(n, tokens, norm_gain, up_weight, down_weight):
    rows, D = tokens.shape
    up_rows, block = up_weight.shape
    H = block // 2
    CW = CHUNK_COLS
    DC = down_weight.shape[1] // CW
    total = n * DC
    own_rows = rows // 4
    bf, f32 = jnp.bfloat16, jnp.float32
    dma = pltpu.SemaphoreType.DMA
    return pl.pallas_call(
        functools.partial(kernel, n),
        out_shape=jax.ShapeDtypeStruct((own_rows, D), bf),
        in_specs=[
            pl.BlockSpec(memory_space=pl.ANY),
            pl.BlockSpec(memory_space=pltpu.VMEM),
            pl.BlockSpec(memory_space=pl.ANY),
            pl.BlockSpec(memory_space=pl.ANY),
        ],
        out_specs=pl.BlockSpec(memory_space=pl.ANY),
        scratch_shapes=[
            pltpu.VMEM((2, rows, D), bf),
            pltpu.VMEM((2 * rows, D), bf),
            pltpu.VMEM((n * up_rows, H), bf),
            pltpu.VMEM((n * DC, H, CW), bf),
            pltpu.VMEM((2 * rows, H), bf),
            pltpu.VMEM((rows, CW), f32),
            pltpu.VMEM((total, own_rows, CW), f32),
            pltpu.VMEM((total, rows, CW), bf),
            pltpu.VMEM((total, rows, CW), bf),
            pltpu.VMEM((total, 4, own_rows, CW), bf),
            pltpu.VMEM((total, 3, own_rows, CW), bf),
            pltpu.VMEM((total, own_rows, CW), bf),
            dma((2, n * UP_CHUNKS)),
            dma((n * UP_CHUNKS,)),
            dma((2, n * DC)),
            dma((n * DC,)),
            dma((2,)),
            dma((2,)),
            dma((total,)),
            dma((total,)),
            dma((total, 3)),
            dma((total, 3)),
            dma((1 + UP_CHUNKS + DC,)),
            dma((total,)),
        ],
        compiler_params=pltpu.CompilerParams(
            collective_id=0, has_side_effects=True, vmem_limit_bytes=58 * 1024 * 1024
        ),
    )(tokens, norm_gain.reshape(1, D), up_weight, down_weight)


def fits(mesh, tokens, up_weight, down_weight):
    n = mesh.shape["fs"]
    rows = tokens.shape[0] // (mesh.shape["rep"] * n)
    columns = down_weight.shape[1] // n
    depth = up_weight.shape[0] // n
    hidden = up_weight.shape[1] // mesh.shape["tp"]
    return (
        mesh.shape["rep"] == 2
        and mesh.shape["tp"] == 4
        and n <= 8
        and columns % CHUNK_COLS == 0
        and depth % (UP_CHUNKS * 16) == 0
        and hidden % 256 == 0
        and rows % 64 == 0
        and rows <= 512
        and hidden <= 1024
        and tokens.shape[1] <= 2048
    )


def solution(mesh):
    placed = (P(("rep", "fs"), None), P(), P("fs", "tp"), P("tp", "fs"))

    def layer(tokens, norm_gain, up_weight, down_weight):
        if fits(mesh, tokens, up_weight, down_weight):
            body = functools.partial(fused, mesh.shape["fs"])
        else:
            body = shards
        return jax.shard_map(
            body, mesh=mesh, in_specs=placed, out_specs=P(("rep", "fs", "tp"), None), check_vma=False
        )(tokens, norm_gain, up_weight, down_weight)

    return layer
```

```python
import functools

import jax
import jax.numpy as jnp
from jax import lax
from jax.experimental import pallas as pl
from jax.experimental.pallas import tpu as pltpu
from jax.sharding import PartitionSpec as P

EPS = 1e-06
UP_CHUNKS = 2
CHUNK_COLS = 128
LAG = 4


def shards(tokens, norm_gain, up_weight, down_weight):
    xf = tokens.astype(jnp.float32)
    scale = lax.rsqrt(jnp.mean(xf * xf, axis=-1, keepdims=True) + EPS)
    normed = (xf * scale * norm_gain).astype(jnp.bfloat16)
    rows = tokens.shape[0]
    halves = lax.axis_size("rep")
    share = up_weight.shape[0] // halves
    mine = lax.dynamic_slice_in_dim(up_weight, lax.axis_index("rep") * share, share, 0)
    arranged = normed.reshape(rows, -1, halves, share).transpose(0, 2, 1, 3).reshape(rows, -1)
    lifted = jnp.dot(
        arranged,
        lax.all_gather(mine, ("rep", "fs"), axis=0, tiled=True),
        preferred_element_type=jnp.float32,
    )
    width = down_weight.shape[1] // halves
    down_mine = lax.dynamic_slice_in_dim(down_weight, lax.axis_index("rep") * width, width, 1)
    collected = lax.all_gather(down_mine, ("rep", "fs"), axis=1, tiled=True)
    hidden_rows = collected.shape[0]
    down_block = (
        collected.reshape(hidden_rows, halves, -1, width)
        .transpose(0, 2, 1, 3)
        .reshape(hidden_rows, -1)
    )
    hidden = jnp.square(jnp.maximum(lifted, 0.0)).astype(jnp.bfloat16)
    own_rows = rows // lax.axis_size("tp")
    summed = lax.psum_scatter(
        jnp.dot(hidden, down_block, preferred_element_type=jnp.float32).astype(jnp.bfloat16),
        "tp",
        scatter_dimension=0,
        tiled=True,
    ).astype(jnp.float32)
    residual = lax.dynamic_slice_in_dim(xf, lax.axis_index("tp") * own_rows, own_rows, 0)
    return (residual + summed).astype(jnp.bfloat16)


def kernel(
    n, tok_hbm, gain_hbm, up_hbm, dn_hbm, out_hbm,
    gain_ref, tok, nrm, upw, dnw, hid, acc, keep, asend, arecv, bsend, brecv, outv,
    up_send, up_recv, dn_send, dn_recv, tok_send, tok_recv,
    a_send, a_recv, b_send, b_recv, local, out_sem,
):
    y, z, t = lax.axis_index("rep"), lax.axis_index("fs"), lax.axis_index("tp")
    x, core = t // 2, t % 2
    partner = x * 2 + (1 - core)
    rows = tok_hbm.shape[0]
    own_rows = rows // 4
    up_rows = up_hbm.shape[0]
    H = upw.shape[1]
    CW = dnw.shape[2]
    DC = dn_hbm.shape[1] // CW
    UC = UP_CHUNKS
    piece = up_rows // UC
    half = rows // 2
    total = n * DC

    def at(yy, zz, tt):
        return {"rep": yy, "fs": zz, "tp": tt}

    def remote(src, dst, send, recv, where):
        return pltpu.make_async_remote_copy(
            src_ref=src, dst_ref=dst, send_sem=send, recv_sem=recv,
            device_id=where, device_id_type=pl.DeviceIdType.MESH,
        )

    def beside(side):
        return at(y, z - 1 if side == 0 else z + 1, t)

    def up_slot(s, c):
        return upw.at[pl.ds(pl.multiple_of(s * up_rows + c * piece, piece), piece), :]

    def up_own(c):
        return up_hbm.at[pl.ds(c * piece, piece), pl.ds(pl.multiple_of(y * H, H), H)]

    def dn_own(c):
        return dn_hbm.at[pl.ds(pl.multiple_of(y * H, H), H), pl.ds(c * CW, CW)]

    def up_copy(side, s, c, src):
        return remote(src, up_slot(s, c), up_send.at[side, s * UC + c],
                      up_recv.at[s * UC + c], beside(side))

    def dn_copy(side, s, c, src):
        return remote(src, dnw.at[s * DC + c], dn_send.at[side, s * DC + c],
                      dn_recv.at[s * DC + c], beside(side))

    def send_own_dn(side):
        for c in range(DC):
            dn_copy(side, z, c, dnw.at[z * DC + c]).start()

    def source(p):
        m = jnp.minimum(z, n - 1 - z)
        k = jnp.where(p <= 2 * m, (p + 1) // 2, p - m)
        sign = jnp.where(
            p <= 2 * m, jnp.where(p % 2 == 1, 1, -1), jnp.where(z < n - 1 - z, 1, -1)
        )
        return z + sign * k

    peers = [at(y, z, partner)]
    for j in (1, 2, 3):
        peers.append(at((y + j // 2) % 2, z, ((x + j % 2) % 2) * 2 + core))
    barrier = pltpu.get_barrier_semaphore()
    for peer in peers:
        pl.semaphore_signal(barrier, inc=1, device_id=peer, device_id_type=pl.DeviceIdType.MESH)
    has = (z > 0, z < n - 1)
    for side in (0, 1):
        @pl.when(has[side])
        def _():
            pl.semaphore_signal(
                barrier, inc=1, device_id=beside(side), device_id_type=pl.DeviceIdType.MESH
            )
    up_loads = [
        pltpu.make_async_copy(up_own(c), up_slot(z, c), local.at[c]) for c in range(UC)
    ]
    dn_loads = [
        pltpu.make_async_copy(dn_own(c), dnw.at[z * DC + c], local.at[UC + c]) for c in range(DC)
    ]
    tok_load = pltpu.make_async_copy(tok_hbm, tok.at[y], local.at[UC + DC])
    gain_load = pltpu.make_async_copy(gain_hbm, gain_ref, local.at[UC + DC + 1])
    for load in up_loads + dn_loads + [gain_load, tok_load]:
        load.start()

    greeted = 4 + jnp.where(has[0], 1, 0) + jnp.where(has[1], 1, 0)
    pl.semaphore_wait(barrier, greeted)

    for c in range(UC):
        up_loads[c].wait()
        for side in (0, 1):
            @pl.when(has[side])
            def _():
                up_copy(side, z, c, up_slot(z, c)).start()

    part = pl.ds(pl.multiple_of(core * half, half), half)
    across = remote(tok_hbm.at[part, :], tok.at[y, part, :], tok_send.at[0], tok_recv.at[0],
                    at(1 - y, z, t))
    across.start()
    for load in dn_loads:
        load.wait()

    @pl.when(z == 0)
    def _():
        send_own_dn(1)

    @pl.when(z == n - 1)
    def _():
        send_own_dn(0)

    gain_load.wait()
    gain = gain_ref[...]

    def normalise(yy):
        def tile(i, carry):
            xf = tok[yy, pl.ds(pl.multiple_of(i * own_rows, own_rows), own_rows), :].astype(jnp.float32)
            scale = lax.rsqrt(jnp.mean(xf * xf, axis=-1, keepdims=True) + EPS)
            to = (i % 2) * rows + (yy * 2 + i // 2) * own_rows
            nrm[pl.ds(pl.multiple_of(to, own_rows), own_rows), :] = (xf * scale * gain).astype(jnp.bfloat16)
            return carry
        lax.fori_loop(0, 4, tile, 0)

    tok_load.wait()
    normalise(y)

    for p in range(1, n):
        s = source(p)
        for c in range(UC):
            up_copy(0, s, c, up_slot(s, c)).wait_recv()
            for side in (0, 1):
                @pl.when(((s > z) if side == 0 else (s < z)) & has[side])
                def _():
                    up_copy(side, s, c, up_slot(s, c)).start()
        for side in (0, 1):
            @pl.when((s == (n - 1 if side == 0 else 0)) & has[side])
            def _():
                send_own_dn(side)

    theirs = pl.ds(pl.multiple_of((1 - core) * half, half), half)
    across.wait_recv()
    over = remote(tok.at[1 - y, part, :], tok.at[1 - y, part, :], tok_send.at[1], tok_recv.at[1],
                  at(y, z, partner))
    over.start()
    remote(tok.at[1 - y, theirs, :], tok.at[1 - y, theirs, :], tok_send.at[1], tok_recv.at[1],
           at(y, z, partner)).wait_recv()
    normalise(1 - y)

    def lift(i, carry):
        r = pl.ds(pl.multiple_of(i * half, half), half)
        lifted = jnp.dot(nrm[r, :], upw[...], preferred_element_type=jnp.float32)
        hid[r, :] = jnp.square(jnp.maximum(lifted, 0.0)).astype(jnp.bfloat16)
        return carry

    lax.fori_loop(0, 2 * rows // half, lift, 0)

    own_q = y * 2 + x

    def a_copy(i):
        return remote(asend.at[i], arecv.at[i], a_send.at[i], a_recv.at[i], at(y, z, partner))

    def b_copy(i, j):
        yy, xx = (y + j // 2) % 2, (x + j % 2) % 2
        return remote(bsend.at[i, yy * 2 + xx], brecv.at[i, j - 1], b_send.at[i, j - 1],
                      b_recv.at[i, j - 1], at(yy, z, xx * 2 + core))

    def out_copy(i):
        column = (source(i // DC) * DC + i % DC) * CW
        return pltpu.make_async_copy(
            outv.at[i], out_hbm.at[:, pl.ds(pl.multiple_of(column, CW), CW)], out_sem.at[i]
        )

    def finish(i):
        for j in (1, 2, 3):
            b_copy(i, j).wait_recv()
        column = (source(i // DC) * DC + i % DC) * CW
        res = tok[y, pl.ds(pl.multiple_of(t * own_rows, own_rows), own_rows),
                  pl.ds(pl.multiple_of(column, CW), CW)].astype(jnp.float32)
        res = res + keep[i]
        for j in range(3):
            res = res + brecv[i, j].astype(jnp.float32)
        outv[i] = res.astype(jnp.bfloat16)
        out_copy(i).start()

    def step(i, carry):
        p, c = i // DC, i % DC
        s = source(p)

        @pl.when(p > 0)
        def _():
            dn_copy(0, s, c, dnw.at[s * DC + c]).wait_recv()
            for side in (0, 1):
                @pl.when(((s > z) if side == 0 else (s < z)) & has[side])
                def _():
                    dn_copy(side, s, c, dnw.at[s * DC + c]).start()

        block = dnw[s * DC + c]
        first = hid[pl.ds(pl.multiple_of((1 - core) * rows, rows), rows), :]
        asend[i] = jnp.dot(first, block, preferred_element_type=jnp.float32).astype(jnp.bfloat16)
        a_copy(i).start()
        second = hid[pl.ds(pl.multiple_of(core * rows, rows), rows), :]
        acc[i % 2] = jnp.dot(second, block, preferred_element_type=jnp.float32)

        @pl.when(i > 0)
        def _():
            join(i - 1)

        @pl.when(i >= LAG)
        def _():
            finish(i - LAG)
        return carry

    def join(i):
        a_copy(i).wait_recv()
        for q in range(4):
            r = pl.ds(q * own_rows, own_rows)
            bsend[i, q] = (acc[i % 2, r, :] + arecv[i, r, :].astype(jnp.float32)).astype(jnp.bfloat16)
        for j in (3, 2, 1):
            b_copy(i, j).start()
        r = pl.ds(pl.multiple_of(own_q * own_rows, own_rows), own_rows)
        keep[i] = acc[i % 2, r, :] + arecv[i, r, :].astype(jnp.float32)

    lax.fori_loop(0, total, step, 0)
    join(total - 1)
    for i in range(total - LAG, total):
        finish(i)

    across.wait_send()
    over.wait_send()

    def drain(i, carry):
        a_copy(i).wait_send()
        for j in (1, 2, 3):
            b_copy(i, j).wait_send()
        out_copy(i).wait()
        return carry

    lax.fori_loop(0, total, drain, 0)
    for side in (0, 1):
        for s in range(n):
            @pl.when(((z <= s) if side == 0 else (z >= s)) & has[side])
            def _():
                for c in range(UC):
                    up_copy(side, s, c, up_slot(s, c)).wait_send()
                for c in range(DC):
                    dn_copy(side, s, c, dnw.at[s * DC + c]).wait_send()


def fused(n, tokens, norm_gain, up_weight, down_weight):
    rows, D = tokens.shape
    up_rows, block = up_weight.shape
    H = block // 2
    CW = CHUNK_COLS
    DC = down_weight.shape[1] // CW
    total = n * DC
    own_rows = rows // 4
    bf, f32 = jnp.bfloat16, jnp.float32
    dma = pltpu.SemaphoreType.DMA
    return pl.pallas_call(
        functools.partial(kernel, n),
        out_shape=jax.ShapeDtypeStruct((own_rows, D), bf),
        in_specs=[
            pl.BlockSpec(memory_space=pl.ANY),
            pl.BlockSpec(memory_space=pl.ANY),
            pl.BlockSpec(memory_space=pl.ANY),
            pl.BlockSpec(memory_space=pl.ANY),
        ],
        out_specs=pl.BlockSpec(memory_space=pl.ANY),
        scratch_shapes=[
            pltpu.VMEM((1, D), f32),
            pltpu.VMEM((2, rows, D), bf),
            pltpu.VMEM((2 * rows, D), bf),
            pltpu.VMEM((n * up_rows, H), bf),
            pltpu.VMEM((n * DC, H, CW), bf),
            pltpu.VMEM((2 * rows, H), bf),
            pltpu.VMEM((2, rows, CW), f32),
            pltpu.VMEM((total, own_rows, CW), f32),
            pltpu.VMEM((total, rows, CW), bf),
            pltpu.VMEM((total, rows, CW), bf),
            pltpu.VMEM((total, 4, own_rows, CW), bf),
            pltpu.VMEM((total, 3, own_rows, CW), bf),
            pltpu.VMEM((total, own_rows, CW), bf),
            dma((2, n * UP_CHUNKS)),
            dma((n * UP_CHUNKS,)),
            dma((2, n * DC)),
            dma((n * DC,)),
            dma((2,)),
            dma((2,)),
            dma((total,)),
            dma((total,)),
            dma((total, 3)),
            dma((total, 3)),
            dma((2 + UP_CHUNKS + DC,)),
            dma((total,)),
        ],
        compiler_params=pltpu.CompilerParams(
            collective_id=0, has_side_effects=True, vmem_limit_bytes=53 * 1024 * 1024
        ),
    )(tokens, norm_gain.reshape(1, D), up_weight, down_weight)


def fits(mesh, tokens, up_weight, down_weight):
    n = mesh.shape["fs"]
    rows = tokens.shape[0] // (mesh.shape["rep"] * n)
    columns = down_weight.shape[1] // n
    depth = up_weight.shape[0] // n
    hidden = up_weight.shape[1] // mesh.shape["tp"]
    return (
        mesh.shape["rep"] == 2
        and mesh.shape["tp"] == 4
        and n <= 8
        and columns % CHUNK_COLS == 0
        and depth % (UP_CHUNKS * 16) == 0
        and hidden % 256 == 0
        and rows % 64 == 0
        and rows <= 512
        and hidden <= 1024
        and tokens.shape[1] <= 2048
    )


def solution(mesh):
    placed = (P(("rep", "fs"), None), P(), P("fs", "tp"), P("tp", "fs"))

    def layer(tokens, norm_gain, up_weight, down_weight):
        if fits(mesh, tokens, up_weight, down_weight):
            body = functools.partial(fused, mesh.shape["fs"])
        else:
            body = shards
        return jax.shard_map(
            body, mesh=mesh, in_specs=placed, out_specs=P(("rep", "fs", "tp"), None), check_vma=False
        )(tokens, norm_gain, up_weight, down_weight)

    return layer
```

```python
import functools

import jax
import jax.numpy as jnp
from jax import lax
from jax.experimental import pallas as pl
from jax.experimental.pallas import tpu as pltpu
from jax.sharding import PartitionSpec as P

EPS = 1e-06
UP_CHUNKS = 2
CHUNK_COLS = 128
LAG = 4


def shards(tokens, norm_gain, up_weight, down_weight):
    xf = tokens.astype(jnp.float32)
    scale = lax.rsqrt(jnp.mean(xf * xf, axis=-1, keepdims=True) + EPS)
    normed = (xf * scale * norm_gain).astype(jnp.bfloat16)
    rows = tokens.shape[0]
    halves = lax.axis_size("rep")
    share = up_weight.shape[0] // halves
    mine = lax.dynamic_slice_in_dim(up_weight, lax.axis_index("rep") * share, share, 0)
    arranged = normed.reshape(rows, -1, halves, share).transpose(0, 2, 1, 3).reshape(rows, -1)
    lifted = jnp.dot(
        arranged,
        lax.all_gather(mine, ("rep", "fs"), axis=0, tiled=True),
        preferred_element_type=jnp.float32,
    )
    width = down_weight.shape[1] // halves
    down_mine = lax.dynamic_slice_in_dim(down_weight, lax.axis_index("rep") * width, width, 1)
    collected = lax.all_gather(down_mine, ("rep", "fs"), axis=1, tiled=True)
    hidden_rows = collected.shape[0]
    down_block = (
        collected.reshape(hidden_rows, halves, -1, width)
        .transpose(0, 2, 1, 3)
        .reshape(hidden_rows, -1)
    )
    hidden = jnp.square(jnp.maximum(lifted, 0.0)).astype(jnp.bfloat16)
    own_rows = rows // lax.axis_size("tp")
    summed = lax.psum_scatter(
        jnp.dot(hidden, down_block, preferred_element_type=jnp.float32).astype(jnp.bfloat16),
        "tp",
        scatter_dimension=0,
        tiled=True,
    ).astype(jnp.float32)
    residual = lax.dynamic_slice_in_dim(xf, lax.axis_index("tp") * own_rows, own_rows, 0)
    return (residual + summed).astype(jnp.bfloat16)


def kernel(
    n, tok_hbm, gain_hbm, up_hbm, dn_hbm, out_hbm,
    gain_ref, tok, nrm, upw, dnw, hid, acc, keep, asend, arecv, bsend, brecv, outv,
    up_send, up_recv, dn_send, dn_recv, tok_send, tok_recv,
    a_send, a_recv, b_send, b_recv, local, out_sem,
):
    y, z, t = lax.axis_index("rep"), lax.axis_index("fs"), lax.axis_index("tp")
    x, core = t // 2, t % 2
    partner = x * 2 + (1 - core)
    rows = tok_hbm.shape[0]
    own_rows = rows // 4
    up_rows = up_hbm.shape[0]
    H = upw.shape[1]
    CW = dnw.shape[2]
    DC = dn_hbm.shape[1] // CW
    UC = UP_CHUNKS
    piece = up_rows // UC
    half = rows // 2
    total = n * DC

    def at(yy, zz, tt):
        return {"rep": yy, "fs": zz, "tp": tt}

    def remote(src, dst, send, recv, where):
        return pltpu.make_async_remote_copy(
            src_ref=src, dst_ref=dst, send_sem=send, recv_sem=recv,
            device_id=where, device_id_type=pl.DeviceIdType.MESH,
        )

    def beside(side):
        return at(y, z - 1 if side == 0 else z + 1, t)

    def up_slot(s, c):
        return upw.at[pl.ds(pl.multiple_of(s * up_rows + c * piece, piece), piece), :]

    def up_own(c):
        return up_hbm.at[pl.ds(c * piece, piece), pl.ds(pl.multiple_of(y * H, H), H)]

    def dn_own(c):
        return dn_hbm.at[pl.ds(pl.multiple_of(y * H, H), H), pl.ds(c * CW, CW)]

    def up_copy(side, s, c, src):
        return remote(src, up_slot(s, c), up_send.at[side, s * UC + c],
                      up_recv.at[s * UC + c], beside(side))

    def dn_copy(side, s, c, src):
        return remote(src, dnw.at[s * DC + c], dn_send.at[side, s * DC + c],
                      dn_recv.at[s * DC + c], beside(side))

    def dn_pair(side, s, c):
        two = dnw.at[pl.ds(s * DC + c, 2)]
        return remote(two, two, dn_send.at[side, s * DC + c], dn_recv.at[s * DC + c], beside(side))

    def outer(s):
        return (s == 0) | (s == n - 1)

    def send_own_dn(side):
        @pl.when(outer(z))
        def _():
            for c in range(DC):
                dn_copy(side, z, c, dnw.at[z * DC + c]).start()

        @pl.when(jnp.logical_not(outer(z)))
        def _():
            for c in range(0, DC, 2):
                dn_pair(side, z, c).start()

    def source(p):
        m = jnp.minimum(z, n - 1 - z)
        k = jnp.where(p <= 2 * m, (p + 1) // 2, p - m)
        sign = jnp.where(
            p <= 2 * m, jnp.where(p % 2 == 1, 1, -1), jnp.where(z < n - 1 - z, 1, -1)
        )
        return z + sign * k

    peers = [at(y, z, partner)]
    for j in (1, 2, 3):
        peers.append(at((y + j // 2) % 2, z, ((x + j % 2) % 2) * 2 + core))
    barrier = pltpu.get_barrier_semaphore()
    for peer in peers:
        pl.semaphore_signal(barrier, inc=1, device_id=peer, device_id_type=pl.DeviceIdType.MESH)
    has = (z > 0, z < n - 1)
    for side in (0, 1):
        @pl.when(has[side])
        def _():
            pl.semaphore_signal(
                barrier, inc=1, device_id=beside(side), device_id_type=pl.DeviceIdType.MESH
            )
    up_loads = [
        pltpu.make_async_copy(up_own(c), up_slot(z, c), local.at[c]) for c in range(UC)
    ]
    dn_loads = [
        pltpu.make_async_copy(dn_own(c), dnw.at[z * DC + c], local.at[UC + c]) for c in range(DC)
    ]
    tok_load = pltpu.make_async_copy(tok_hbm, tok.at[y], local.at[UC + DC])
    gain_load = pltpu.make_async_copy(gain_hbm, gain_ref, local.at[UC + DC + 1])
    for load in up_loads + dn_loads + [gain_load, tok_load]:
        load.start()

    greeted = 4 + jnp.where(has[0], 1, 0) + jnp.where(has[1], 1, 0)
    pl.semaphore_wait(barrier, greeted)

    for c in range(UC):
        up_loads[c].wait()
        for side in (0, 1):
            @pl.when(has[side])
            def _():
                up_copy(side, z, c, up_slot(z, c)).start()

    part = pl.ds(pl.multiple_of(core * half, half), half)
    across = remote(tok_hbm.at[part, :], tok.at[y, part, :], tok_send.at[0], tok_recv.at[0],
                    at(1 - y, z, t))
    across.start()
    for load in dn_loads:
        load.wait()

    @pl.when(z == 0)
    def _():
        send_own_dn(1)

    @pl.when(z == n - 1)
    def _():
        send_own_dn(0)

    gain_load.wait()
    gain = gain_ref[...]

    def normalise(yy):
        def tile(i, carry):
            xf = tok[yy, pl.ds(pl.multiple_of(i * own_rows, own_rows), own_rows), :].astype(jnp.float32)
            scale = lax.rsqrt(jnp.mean(xf * xf, axis=-1, keepdims=True) + EPS)
            to = (i % 2) * rows + (yy * 2 + i // 2) * own_rows
            nrm[pl.ds(pl.multiple_of(to, own_rows), own_rows), :] = (xf * scale * gain).astype(jnp.bfloat16)
            return carry
        lax.fori_loop(0, 4, tile, 0)

    tok_load.wait()
    normalise(y)

    for p in range(1, n):
        s = source(p)
        for c in range(UC):
            up_copy(0, s, c, up_slot(s, c)).wait_recv()
            for side in (0, 1):
                @pl.when(((s > z) if side == 0 else (s < z)) & has[side])
                def _():
                    up_copy(side, s, c, up_slot(s, c)).start()
        for side in (0, 1):
            @pl.when((s == (n - 1 if side == 0 else 0)) & has[side])
            def _():
                send_own_dn(side)

    theirs = pl.ds(pl.multiple_of((1 - core) * half, half), half)
    across.wait_recv()
    over = remote(tok.at[1 - y, part, :], tok.at[1 - y, part, :], tok_send.at[1], tok_recv.at[1],
                  at(y, z, partner))
    over.start()
    remote(tok.at[1 - y, theirs, :], tok.at[1 - y, theirs, :], tok_send.at[1], tok_recv.at[1],
           at(y, z, partner)).wait_recv()
    normalise(1 - y)

    def lift(i, carry):
        r = pl.ds(pl.multiple_of(i * half, half), half)
        lifted = jnp.dot(nrm[r, :], upw[...], preferred_element_type=jnp.float32)
        hid[r, :] = jnp.square(jnp.maximum(lifted, 0.0)).astype(jnp.bfloat16)
        return carry

    lax.fori_loop(0, 2 * rows // half, lift, 0)

    own_q = y * 2 + x

    def a_copy(i):
        return remote(asend.at[i], arecv.at[i], a_send.at[i], a_recv.at[i], at(y, z, partner))

    def b_copy(i, j):
        yy, xx = (y + j // 2) % 2, (x + j % 2) % 2
        return remote(bsend.at[i, yy * 2 + xx], brecv.at[i, j - 1], b_send.at[i, j - 1],
                      b_recv.at[i, j - 1], at(yy, z, xx * 2 + core))

    def out_copy(i):
        column = (source(i // DC) * DC + i % DC) * CW
        return pltpu.make_async_copy(
            outv.at[i], out_hbm.at[:, pl.ds(pl.multiple_of(column, CW), CW)], out_sem.at[i]
        )

    def finish(i):
        for j in (1, 2, 3):
            b_copy(i, j).wait_recv()
        column = (source(i // DC) * DC + i % DC) * CW
        res = tok[y, pl.ds(pl.multiple_of(t * own_rows, own_rows), own_rows),
                  pl.ds(pl.multiple_of(column, CW), CW)].astype(jnp.float32)
        res = res + keep[i]
        for j in range(3):
            res = res + brecv[i, j].astype(jnp.float32)
        outv[i] = res.astype(jnp.bfloat16)
        out_copy(i).start()

    def step(i, carry):
        p, c = i // DC, i % DC
        s = source(p)

        @pl.when((p > 0) & outer(s))
        def _():
            dn_copy(0, s, c, dnw.at[s * DC + c]).wait_recv()
            for side in (0, 1):
                @pl.when(((s > z) if side == 0 else (s < z)) & has[side])
                def _():
                    dn_copy(side, s, c, dnw.at[s * DC + c]).start()

        @pl.when((p > 0) & jnp.logical_not(outer(s)) & (c % 2 == 0))
        def _():
            dn_pair(0, s, c).wait_recv()
            for side in (0, 1):
                @pl.when(((s > z) if side == 0 else (s < z)) & has[side])
                def _():
                    dn_pair(side, s, c).start()

        block = dnw[s * DC + c]
        first = hid[pl.ds(pl.multiple_of((1 - core) * rows, rows), rows), :]
        asend[i] = jnp.dot(first, block, preferred_element_type=jnp.float32).astype(jnp.bfloat16)
        a_copy(i).start()
        second = hid[pl.ds(pl.multiple_of(core * rows, rows), rows), :]
        acc[i % 2] = jnp.dot(second, block, preferred_element_type=jnp.float32)

        @pl.when(i > 0)
        def _():
            join(i - 1)

        @pl.when(i >= LAG)
        def _():
            finish(i - LAG)
        return carry

    def join(i):
        a_copy(i).wait_recv()
        for q in range(4):
            r = pl.ds(q * own_rows, own_rows)
            bsend[i, q] = (acc[i % 2, r, :] + arecv[i, r, :].astype(jnp.float32)).astype(jnp.bfloat16)
        for j in (3, 2, 1):
            b_copy(i, j).start()
        r = pl.ds(pl.multiple_of(own_q * own_rows, own_rows), own_rows)
        keep[i] = acc[i % 2, r, :] + arecv[i, r, :].astype(jnp.float32)

    lax.fori_loop(0, total, step, 0)
    join(total - 1)
    for i in range(total - LAG, total - 1):
        finish(i)

    across.wait_send()
    over.wait_send()
    for side in (0, 1):
        for s in range(n):
            @pl.when(((z <= s) if side == 0 else (z >= s)) & has[side])
            def _():
                for c in range(UC):
                    up_copy(side, s, c, up_slot(s, c)).wait_send()
                if s in (0, n - 1):
                    for c in range(DC):
                        dn_copy(side, s, c, dnw.at[s * DC + c]).wait_send()
                else:
                    for c in range(0, DC, 2):
                        dn_pair(side, s, c).wait_send()

    def drain(i, carry):
        a_copy(i).wait_send()
        for j in (1, 2, 3):
            b_copy(i, j).wait_send()
        out_copy(i).wait()
        return carry

    lax.fori_loop(0, total - 1, drain, 0)
    finish(total - 1)
    drain(total - 1, 0)


def fused(n, tokens, norm_gain, up_weight, down_weight):
    rows, D = tokens.shape
    up_rows, block = up_weight.shape
    H = block // 2
    CW = CHUNK_COLS
    DC = down_weight.shape[1] // CW
    total = n * DC
    own_rows = rows // 4
    bf, f32 = jnp.bfloat16, jnp.float32
    dma = pltpu.SemaphoreType.DMA
    return pl.pallas_call(
        functools.partial(kernel, n),
        out_shape=jax.ShapeDtypeStruct((own_rows, D), bf),
        in_specs=[
            pl.BlockSpec(memory_space=pl.ANY),
            pl.BlockSpec(memory_space=pl.ANY),
            pl.BlockSpec(memory_space=pl.ANY),
            pl.BlockSpec(memory_space=pl.ANY),
        ],
        out_specs=pl.BlockSpec(memory_space=pl.ANY),
        scratch_shapes=[
            pltpu.VMEM((1, D), f32),
            pltpu.VMEM((2, rows, D), bf),
            pltpu.VMEM((2 * rows, D), bf),
            pltpu.VMEM((n * up_rows, H), bf),
            pltpu.VMEM((n * DC, H, CW), bf),
            pltpu.VMEM((2 * rows, H), bf),
            pltpu.VMEM((2, rows, CW), f32),
            pltpu.VMEM((total, own_rows, CW), f32),
            pltpu.VMEM((total, rows, CW), bf),
            pltpu.VMEM((total, rows, CW), bf),
            pltpu.VMEM((total, 4, own_rows, CW), bf),
            pltpu.VMEM((total, 3, own_rows, CW), bf),
            pltpu.VMEM((total, own_rows, CW), bf),
            dma((2, n * UP_CHUNKS)),
            dma((n * UP_CHUNKS,)),
            dma((2, n * DC)),
            dma((n * DC,)),
            dma((2,)),
            dma((2,)),
            dma((total,)),
            dma((total,)),
            dma((total, 3)),
            dma((total, 3)),
            dma((2 + UP_CHUNKS + DC,)),
            dma((total,)),
        ],
        compiler_params=pltpu.CompilerParams(
            collective_id=0, has_side_effects=True, vmem_limit_bytes=53 * 1024 * 1024
        ),
    )(tokens, norm_gain.reshape(1, D), up_weight, down_weight)


def fits(mesh, tokens, up_weight, down_weight):
    n = mesh.shape["fs"]
    rows = tokens.shape[0] // (mesh.shape["rep"] * n)
    columns = down_weight.shape[1] // n
    depth = up_weight.shape[0] // n
    hidden = up_weight.shape[1] // mesh.shape["tp"]
    return (
        mesh.shape["rep"] == 2
        and mesh.shape["tp"] == 4
        and n <= 8
        and columns % (2 * CHUNK_COLS) == 0
        and depth % (UP_CHUNKS * 16) == 0
        and hidden % 256 == 0
        and rows % 64 == 0
        and rows <= 512
        and hidden <= 1024
        and tokens.shape[1] <= 2048
    )


def solution(mesh):
    placed = (P(("rep", "fs"), None), P(), P("fs", "tp"), P("tp", "fs"))

    def layer(tokens, norm_gain, up_weight, down_weight):
        if fits(mesh, tokens, up_weight, down_weight):
            body = functools.partial(fused, mesh.shape["fs"])
        else:
            body = shards
        return jax.shard_map(
            body, mesh=mesh, in_specs=placed, out_specs=P(("rep", "fs", "tp"), None), check_vma=False
        )(tokens, norm_gain, up_weight, down_weight)

    return layer
```
